512 devices in a mesh: fs: 128 (over z, y, core), tp: 4 (over x).
Axes of the slice: x: 4, y: 8, z: 8, core: 2. Of those that a mesh axis runs over, the one named last changes fastest.
Arguments:
- inputs: bfloat16 [98304, 2048], P('fs'), may hold values from -6 to 6
- values_cot: bfloat16 [98304, 2048], P('fs', 'tp'), may hold values from -0.057373047 to 0.057373047
- decay_cot: bfloat16 [98304, 16], P('fs'), may hold values from -0.057373047 to 0.057373047
- factor: bfloat16 [2048, 512], P('fs', 'tp'), may hold values from -0.125 to 0.125
- value_weight: float32 [2048, 2048], P('fs', 'tp'), may hold values from -3 to 3
- lowrank_mean: float32 [512, 2048], P('fs', 'tp'), may hold values from -60 to 60
- lowrank_var: float32 [512, 2048], P('fs', 'tp'), may hold values from 0.3 to 3
- decay_weight: float32 [2048, 16], replicated, may hold values from -3 to 3
- decay_mean: float32 [2048, 16], replicated, may hold values from -6 to 6
- decay_var: float32 [2048, 16], replicated, may hold values from 0.3 to 3
Outputs:
- value_step: float32 [2048, 2048], P('fs', 'tp')
- value_new: float32 [2048, 2048], P('fs', 'tp')
- value_copy: bfloat16 [2048, 2048], P('fs', 'tp')
- mean_new: float32 [512, 2048], P('fs', 'tp')
- var_new: float32 [512, 2048], P('fs', 'tp')
- decay_new: float32 [2048, 16], replicated
- decay_copy: bfloat16 [2048, 16], replicated
- decay_mean_new: float32 [2048, 16], replicated
- decay_var_new: float32 [2048, 16], replicated
The draws below stay inside these ranges and needn't reach their ends.
All inputs are finite; a program needn't handle non-finite values.
Results may differ from the reference program's by a relative error of at most 0.0042.
Values may be sent and summed in bfloat16 or wider, within the bound.
No kernel may reach another device: no remote copies, remote signals or barrier semaphores. Data moves between devices by JAX's collectives and lax.ppermute only.
A program may use at most 64 MiB of HBM per device.

```python
import math
import jax
import jax.numpy as jnp
from jax import lax

D = 2048
W = 2048
H = 16
R = 512
TOKENS = 98304


def draw_lowrank_mean(key, part):
    base = jnp.clip(jax.random.normal(key, (R, W), jnp.float32), -6.0, 6.0)
    row_scale = 10.0 ** (0.5 * jnp.arange(R, dtype=jnp.float32) / R)
    col_scale = 10.0 ** (0.5 * jnp.arange(W, dtype=jnp.float32) / W)
    return base * row_scale[:, None] * col_scale[None, :]


def steps_of(key, shape, cuts, least, largest):
    level = 1.0
    for axis_at, parts in cuts:
        draws = jax.random.uniform(jax.random.fold_in(jax.random.fold_in(key, 6), axis_at), (parts,), jnp.float32, least / len(cuts), largest / len(cuts))
        level = level * jnp.repeat(jnp.exp(draws), shape[axis_at] // parts).reshape((-1,) + (1,) * (len(shape) - 1 - axis_at))
    return level


def noise(rng, shape, deviation, bound, pieces=(), held_as=jnp.bfloat16):
    entries = deviation * jax.random.normal(rng, shape, jnp.float32)
    if pieces:
        entries = entries * steps_of(rng, shape, pieces, -0.22, 0.18)
    return jnp.clip(entries, -bound, bound).astype(held_as)


def setup_inputs(seed: int = 0) -> dict:
    key_of = jax.random.split(jax.random.key(seed), 11)
    inputs = noise(key_of[0], (TOKENS, D), 1.0, 6.0, ((0, 128),))
    values_cot = noise(key_of[1], (TOKENS, W), (3.0 * TOKENS ** -0.5), 0.057373047, ((0, 128), (1, 4)))
    decay_cot = noise(key_of[2], (TOKENS, H), (3.0 * TOKENS ** -0.5), 0.057373047, ((0, 128),))
    factor = noise(key_of[3], (D, R), D ** -0.5, 0.125, ((0, 128), (1, 4)))
    value_weight = noise(key_of[4], (D, W), 0.5, 3.0, ((0, 128), (1, 4)), jnp.float32)
    lowrank_mean = draw_lowrank_mean(jax.random.fold_in(key_of[10], 71), 0)
    lowrank_var = jnp.clip(jnp.exp(math.log(3.0) - 2.3025851 * jax.random.uniform(key_of[6], (R, W), jnp.float32) ** steps_of(key_of[6], (R, W), ((0, 128), (1, 4)), -0.2, 0.2)), 0.3, 3.0)
    decay_weight = noise(key_of[7], (D, H), 0.5, 3.0, (), jnp.float32)
    decay_mean = noise(key_of[8], (D, H), 1.0, 6.0, (), jnp.float32)
    decay_var = jnp.clip(jnp.exp(jax.random.uniform(key_of[9], (D, H), jnp.float32, math.log(0.3), math.log(3.0))), 0.3, 3.0)
    return {"inputs": inputs, "values_cot": values_cot, "decay_cot": decay_cot, "factor": factor, "value_weight": value_weight, "lowrank_mean": lowrank_mean, "lowrank_var": lowrank_var, "decay_weight": decay_weight, "decay_mean": decay_mean, "decay_var": decay_var}


def reference(inputs, values_cot, decay_cot, factor, value_weight, lowrank_mean, lowrank_var, decay_weight, decay_mean, decay_var):
    projected = jnp.dot(inputs, factor, preferred_element_type=jnp.float32).astype(jnp.bfloat16)
    lowrank_grad = lax.dot_general(projected, values_cot, (((0,), (0,)), ((), ())), preferred_element_type=jnp.float32)
    mean_new = 0.9 * lowrank_mean + 0.1 * lowrank_grad
    var_new = 0.95 * lowrank_var + 0.05 * lowrank_grad * lowrank_grad
    adam_ratio = mean_new / (jnp.sqrt(var_new) + 1e-08)
    root_mean = jnp.sqrt(jnp.sum(adam_ratio * adam_ratio) / (R * W) + 1e-06)
    delta = jnp.dot(factor.astype(jnp.float32), adam_ratio, precision=lax.Precision.HIGHEST)
    value_step = -0.5 / root_mean * delta
    value_new = value_weight + value_step
    value_copy = value_new.astype(jnp.bfloat16)
    decay_grad = lax.dot_general(inputs, decay_cot, (((0,), (0,)), ((), ())), preferred_element_type=jnp.float32)
    decay_mean_new = 0.9 * decay_mean + 0.1 * decay_grad
    decay_var_new = 0.95 * decay_var + 0.05 * decay_grad * decay_grad
    decay_new = decay_weight - 0.5 * decay_mean_new / (jnp.sqrt(decay_var_new) + 1e-08)
    decay_copy = decay_new.astype(jnp.bfloat16)
    return (value_step, value_new, value_copy, mean_new, var_new, decay_new, decay_copy, decay_mean_new, decay_var_new)
```

```python
import functools

import jax
import jax.numpy as jnp
from jax import lax
from jax.experimental import pallas as pl
from jax.experimental.pallas import tpu as pltpu
from jax.sharding import Mesh
from jax.sharding import PartitionSpec as P

D = 2048
W = 2048
R = 512
H = 16
FS = ("z", "y", "c")
PLANE = ("z", "y")
CHIPS = 64
SWAP = [(0, 1), (1, 0)]
BF = jnp.bfloat16
F32 = jnp.float32
VMEM = pl.BlockSpec(memory_space=pltpu.VMEM)


def call(body, outs, count, flops, moved, scratch=()):
    return pl.pallas_call(
        body,
        out_shape=outs,
        in_specs=[VMEM] * count,
        out_specs=jax.tree.map(lambda _: VMEM, outs),
        scratch_shapes=list(scratch),
        compiler_params=pltpu.CompilerParams(vmem_limit_bytes=12 << 20),
        cost_estimate=pl.CostEstimate(flops=flops, bytes_accessed=moved, transcendentals=0),
    )


def shape(dims, dtype):
    return jax.ShapeDtypeStruct(dims, dtype)


def split_pair(pair, axis):
    total = pair + pltpu.roll(pair, 4, axis)
    high = total.astype(BF).astype(F32)
    row = lax.broadcasted_iota(jnp.int32, pair.shape, axis)
    return jnp.where(row < 4, high, total - high)


def decay_body(cot_ref, x_ref, out_ref, rows):
    part = jnp.dot(cot_ref[...], x_ref[...], preferred_element_type=F32)
    high = part.astype(BF).astype(F32)
    low = part - high
    for b in range(D // 128):
        at = (b // 4) * 8 + b % 4
        lanes = slice(b * 128, (b + 1) * 128)
        rows[pl.ds(at, H, stride=32), :] = high[:, lanes]
        rows[pl.ds(at + 4, H, stride=32), :] = low[:, lanes]
    out_ref[...] = rows[...].astype(BF).reshape(CHIPS, 8, 128)


def project_body(x_ref, near_ref, far_ref, own_ref, out_ref, whole):
    core = lax.axis_index("c")
    whole[:, pl.ds(core, 1)] = near_ref[...].reshape(CHIPS, 1, 16, 128)
    whole[:, pl.ds(1 - core, 1)] = far_ref[...].reshape(CHIPS, 1, 16, 128)
    part = jnp.dot(
        x_ref[...], whole[...].reshape(D, 128), preferred_element_type=F32
    ).astype(BF)
    a = lax.broadcasted_iota(jnp.int32, (128, 128), 0)
    lane = lax.broadcasted_iota(jnp.int32, (128, 128), 1)
    half = jnp.where(a < 64, 1 - core, core)
    source = (a & 15) * 8 + half * 4 + ((a >> 4) & 3)
    order = jnp.where(lane == source, 1.0, 0.0).astype(BF)
    turned = lax.dot_general(
        order, part, (((1,), (1,)), ((), ())), preferred_element_type=F32
    ).astype(BF)
    out_ref[0:128, :] = turned
    out_ref[128:144, :] = jnp.zeros((16, 768), BF)
    out_ref[128:144, 0:128] = own_ref[...]


def gradient_body(half, p_ref, v_ref, dec_ref, out_ref, rows):
    for q in range(4):
        part = jnp.dot(
            p_ref[q, half * 64 : half * 64 + 64, :], v_ref[...], preferred_element_type=F32
        )
        for i in range(4):
            for cb in range(4):
                rows[pl.ds(q * 256 + cb * 4 + i, 16, stride=16), :] = part[
                    i * 16 : i * 16 + 16, cb * 128 : cb * 128 + 128
                ]
    out_ref[:, 0:16, :] = rows[...].astype(BF).reshape(CHIPS, 16, 128)
    out_ref[:, 16:24, :] = dec_ref[...]


def pair_body(own_ref, peer_ref, out_ref):
    out_ref[:, 0:16, :] = (
        own_ref[:, 0:16, :].astype(F32) + peer_ref[:, 0:16, :].astype(F32)
    ).astype(BF)
    dec = own_ref[:, 16:24, :].astype(F32) + peer_ref[:, 16:24, :].astype(F32)
    out_ref[:, 16:24, :] = split_pair(dec, 1).astype(BF)


def moment_body(got_ref, mean_ref, var_ref, out_ref, mean_out, var_out, mean_s, var_s):
    for cb in range(4):
        lanes = slice(cb * 128, cb * 128 + 128)
        mean_s[cb * 4 : cb * 4 + 4, :] = mean_ref[:, lanes]
        var_s[cb * 4 : cb * 4 + 4, :] = var_ref[:, lanes]
    grad = jnp.sum(got_ref[:, 0:16, :].astype(F32), axis=0)
    dec = jnp.sum(got_ref[:, 16:24, :].astype(F32), axis=0)
    mean_new = 0.9 * mean_s[...] + 0.1 * grad
    var_new = 0.95 * var_s[...] + 0.05 * grad * grad
    ratio = mean_new / (jnp.sqrt(var_new) + 1e-08)
    mean_s[...] = mean_new
    var_s[...] = var_new
    for cb in range(4):
        lanes = slice(cb * 128, cb * 128 + 128)
        mean_out[:, lanes] = mean_s[cb * 4 : cb * 4 + 4, :]
        var_out[:, lanes] = var_s[cb * 4 : cb * 4 + 4, :]
    out_ref[:, 0:16, :] = jnp.broadcast_to(ratio.astype(BF)[None], (CHIPS, 16, 128))
    out_ref[:, 16:24, :] = jnp.broadcast_to(
        split_pair(dec, 0).astype(BF)[None], (CHIPS, 8, 128)
    )


def spread_body(p_ref, out_ref):
    core = lax.axis_index("c")
    lane = lax.broadcasted_iota(jnp.int32, (128, 256), 0)
    k = lax.broadcasted_iota(jnp.int32, (128, 256), 1)
    column = (lax.broadcasted_iota(jnp.int32, (16, 256), 1) >> 2) & 3
    for side in range(2):
        half = core if side == 0 else 1 - core
        pick = jnp.where(lane == (k >> 4) * 8 + half * 4 + (k & 3), 1.0, 0.0).astype(BF)
        for q in range(4):
            rows = jnp.dot(p_ref[q, 128:144, 0:128], pick, preferred_element_type=F32)
            for cb in range(4):
                out_ref[side, cb * 16 : cb * 16 + 16, q * 256 : q * 256 + 256] = jnp.where(
                    column == cb, rows, 0.0
                ).astype(BF)


def decay_update_body(
    got_ref, weight_ref, mean_ref, var_ref, new_out, copy_out, mean_out, var_out, rows
):
    dec = got_ref[:, 16:24, :].astype(F32)
    rows[...] = (dec + pltpu.roll(dec, 4, 1)).reshape(CHIPS * 8, 128)
    for b in range(D // 128):
        lanes = slice(b * 128, (b + 1) * 128)
        grad = rows[pl.ds((b // 4) * 8 + b % 4, H, stride=32), :]
        mean_new = 0.9 * mean_ref[:, lanes] + 0.1 * grad
        var_new = 0.95 * var_ref[:, lanes] + 0.05 * grad * grad
        new = weight_ref[:, lanes] - 0.5 * mean_new / (jnp.sqrt(var_new) + 1e-08)
        mean_out[:, lanes] = mean_new
        var_out[:, lanes] = var_new
        new_out[:, lanes] = new
        copy_out[:, lanes] = new.astype(BF)


def squares_body(near_ref, far_ref, out_ref):
    near = near_ref[:, 0:16, :].astype(F32)
    far = far_ref[:, 0:16, :].astype(F32)
    sums = jnp.sum(near * near + far * far, axis=0)
    sums = sums[0:8] + sums[8:16]
    out_ref[...] = jnp.broadcast_to(sums[None], (4, 8, 128))


def product_body(rows_ref, near_ref, far_ref, out_ref):
    near = near_ref[:, 0:16, :].reshape(CHIPS * 16, 128)
    far = far_ref[:, 0:16, :].reshape(CHIPS * 16, 128)
    got = jnp.dot(rows_ref[0], near, preferred_element_type=F32) + jnp.dot(
        rows_ref[1], far, preferred_element_type=F32
    )
    for cb in range(4):
        out_ref[:, cb * 128 : cb * 128 + 128] = got[cb * 16 : cb * 16 + 16]


def step_body(squares_ref, delta_ref, weight_ref, step_out, new_out, copy_out):
    root_mean = jnp.sqrt(jnp.sum(squares_ref[...]) / (R * W) + 1e-06)
    step = -0.5 / root_mean * delta_ref[...]
    new = weight_ref[...] + step
    step_out[...] = step
    new_out[...] = new
    copy_out[...] = new.astype(BF)


def local(
    inputs,
    values_cot,
    decay_cot,
    factor,
    value_weight,
    lowrank_mean,
    lowrank_var,
    decay_weight,
    decay_mean,
    decay_var,
):
    chunk = shape((CHIPS, 24, 128), BF)
    near = lax.all_to_all(
        jnp.broadcast_to(factor, (CHIPS, 16, 128)), PLANE, 0, 0, tiled=True
    )
    decay_rows = call(
        decay_body,
        shape((CHIPS, 8, 128), BF),
        2,
        2 * 768 * D * H,
        4 << 20,
        [pltpu.VMEM((512, 128), F32)],
    )(decay_cot.T, inputs)
    far = lax.ppermute(near, "c", SWAP)
    quarter = call(
        project_body,
        shape((144, 768), BF),
        4,
        2 * 768 * D * 128,
        4 << 20,
        [pltpu.VMEM((CHIPS, 2, 16, 128), BF)],
    )(inputs, near, far, factor)
    projected = lax.all_gather(quarter, "x")

    def gradient(half):
        return call(
            functools.partial(gradient_body, half),
            chunk,
            3,
            2 * 768 * 256 * 512,
            2 << 20,
            [pltpu.VMEM((CHIPS * 16, 128), F32)],
        )(projected, values_cot, decay_rows)

    peer = lax.ppermute(gradient(0), "c", SWAP)
    paired = call(pair_body, chunk, 2, 400000, 1 << 20)(gradient(1), peer)
    arrived = lax.all_to_all(paired, PLANE, 0, 0, tiled=True)
    rows = call(spread_body, shape((2, 64, 1024), BF), 1, 8 * 2 * 16 * 128 * 256, 1 << 20)(
        projected
    )
    ratio, mean_new, var_new = call(
        moment_body,
        (chunk, shape((4, 512), F32), shape((4, 512), F32)),
        3,
        400000,
        1 << 20,
        [pltpu.VMEM((16, 128), F32)] * 2,
    )(arrived, lowrank_mean, lowrank_var)
    near = lax.all_to_all(ratio, PLANE, 0, 0, tiled=True)
    far = lax.ppermute(near, "c", SWAP)
    state = shape((H, D), F32)
    decay_new, decay_copy, decay_mean_new, decay_var_new = call(
        decay_update_body,
        (state, shape((H, D), BF), state, state),
        4,
        400000,
        1 << 20,
        [pltpu.VMEM((512, 128), F32)],
    )(near, decay_weight.T, decay_mean.T, decay_var.T)
    squares = call(squares_body, shape((4, 8, 128), F32), 2, 400000, 1 << 20)(near, far)
    squares = lax.all_to_all(squares, "x", 0, 0, tiled=True)
    delta = call(
        product_body, shape((16, 512), F32), 3, 2 * 64 * 2048 * 128, 1 << 20
    )(rows, near, far)
    block = shape((16, 512), F32)
    value_step, value_new, value_copy = call(
        step_body, (block, block, shape((16, 512), BF)), 3, 40000, 100000
    )(squares, delta, value_weight)
    return (
        value_step,
        value_new,
        value_copy,
        mean_new,
        var_new,
        decay_new.T,
        decay_copy.T,
        decay_mean_new.T,
        decay_var_new.T,
    )


def solution(mesh):
    split = Mesh(mesh.devices.reshape(8, 8, 2, mesh.shape["tp"]), ("z", "y", "c", "x"))
    placed = (
        P(FS, None),
        P(FS, "x"),
        P(FS, None),
        P(FS, "x"),
        P(FS, "x"),
        P(FS, "x"),
        P(FS, "x"),
        P(),
        P(),
        P(),
    )
    return jax.shard_map(
        local,
        mesh=split,
        in_specs=placed,
        out_specs=(P(FS, "x"),) * 5 + (P(),) * 4,
        check_vma=False,
    )
```

```python
import functools

import jax
import jax.numpy as jnp
from jax import lax
from jax.experimental import pallas as pl
from jax.experimental.pallas import tpu as pltpu
from jax.sharding import Mesh
from jax.sharding import PartitionSpec as P

D = 2048
W = 2048
R = 512
H = 16
FS = ("z", "y", "c")
PLANE = ("z", "y")
CHIPS = 64
SWAP = [(0, 1), (1, 0)]
BF = jnp.bfloat16
F32 = jnp.float32
VMEM = pl.BlockSpec(memory_space=pltpu.VMEM)


def call(body, outs, count, flops, moved, scratch=()):
    return pl.pallas_call(
        body,
        out_shape=outs,
        in_specs=[VMEM] * count,
        out_specs=jax.tree.map(lambda _: VMEM, outs),
        scratch_shapes=list(scratch),
        compiler_params=pltpu.CompilerParams(vmem_limit_bytes=12 << 20),
        cost_estimate=pl.CostEstimate(flops=flops, bytes_accessed=moved, transcendentals=0),
    )


def shape(dims, dtype):
    return jax.ShapeDtypeStruct(dims, dtype)


def split_pair(pair, axis):
    total = pair + pltpu.roll(pair, 4, axis)
    high = total.astype(BF).astype(F32)
    row = lax.broadcasted_iota(jnp.int32, pair.shape, axis)
    return jnp.where(row < 4, high, total - high)


def decay_body(cot_ref, x_ref, out_ref, rows):
    part = jnp.dot(cot_ref[...], x_ref[...], preferred_element_type=F32)
    high = part.astype(BF).astype(F32)
    low = part - high
    for b in range(D // 128):
        at = (b // 4) * 8 + b % 4
        lanes = slice(b * 128, (b + 1) * 128)
        rows[pl.ds(at, H, stride=32), :] = high[:, lanes]
        rows[pl.ds(at + 4, H, stride=32), :] = low[:, lanes]
    out_ref[...] = rows[...].astype(BF).reshape(CHIPS, 8, 128)


def project_body(x_ref, near_ref, far_ref, own_ref, out_ref, whole):
    core = lax.axis_index("c")
    whole[:, pl.ds(core, 1)] = near_ref[...].reshape(CHIPS, 1, 16, 128)
    whole[:, pl.ds(1 - core, 1)] = far_ref[...].reshape(CHIPS, 1, 16, 128)
    part = jnp.dot(
        x_ref[...], whole[...].reshape(D, 128), preferred_element_type=F32
    ).astype(BF)
    a = lax.broadcasted_iota(jnp.int32, (128, 128), 0)
    lane = lax.broadcasted_iota(jnp.int32, (128, 128), 1)
    half = jnp.where(a < 64, 1 - core, core)
    source = (a & 15) * 8 + half * 4 + ((a >> 4) & 3)
    order = jnp.where(lane == source, 1.0, 0.0).astype(BF)
    turned = lax.dot_general(
        order, part, (((1,), (1,)), ((), ())), preferred_element_type=F32
    ).astype(BF)
    out_ref[0:128, :] = turned
    out_ref[128:144, :] = jnp.zeros((16, 768), BF)
    out_ref[128:144, 0:128] = own_ref[...]


def gradient_body(half, p_ref, v_ref, dec_ref, out_ref, rows):
    for q in range(4):
        part = jnp.dot(
            p_ref[q, half * 64 : half * 64 + 64, :], v_ref[...], preferred_element_type=F32
        )
        for i in range(4):
            for cb in range(4):
                rows[pl.ds(q * 256 + cb * 4 + i, 16, stride=16), :] = part[
                    i * 16 : i * 16 + 16, cb * 128 : cb * 128 + 128
                ]
    out_ref[:, 0:16, :] = rows[...].astype(BF).reshape(CHIPS, 16, 128)
    out_ref[:, 16:24, :] = dec_ref[...]


def pair_body(own_ref, peer_ref, out_ref):
    out_ref[:, 0:16, :] = (
        own_ref[:, 0:16, :].astype(F32) + peer_ref[:, 0:16, :].astype(F32)
    ).astype(BF)
    dec = own_ref[:, 16:24, :].astype(F32) + peer_ref[:, 16:24, :].astype(F32)
    out_ref[:, 16:24, :] = split_pair(dec, 1).astype(BF)


def moment_body(got_ref, mean_ref, var_ref, out_ref, mean_out, var_out, mean_s, var_s):
    for cb in range(4):
        lanes = slice(cb * 128, cb * 128 + 128)
        mean_s[cb * 4 : cb * 4 + 4, :] = mean_ref[:, lanes]
        var_s[cb * 4 : cb * 4 + 4, :] = var_ref[:, lanes]
    grad = jnp.sum(got_ref[:, 0:16, :].astype(F32), axis=0)
    dec = jnp.sum(got_ref[:, 16:24, :].astype(F32), axis=0)
    mean_new = 0.9 * mean_s[...] + 0.1 * grad
    var_new = 0.95 * var_s[...] + 0.05 * grad * grad
    ratio = mean_new / (jnp.sqrt(var_new) + 1e-08)
    mean_s[...] = mean_new
    var_s[...] = var_new
    for cb in range(4):
        lanes = slice(cb * 128, cb * 128 + 128)
        mean_out[:, lanes] = mean_s[cb * 4 : cb * 4 + 4, :]
        var_out[:, lanes] = var_s[cb * 4 : cb * 4 + 4, :]
    out_ref[:, 0:16, :] = jnp.broadcast_to(ratio.astype(BF)[None], (CHIPS, 16, 128))
    out_ref[:, 16:24, :] = jnp.broadcast_to(
        split_pair(dec, 0).astype(BF)[None], (CHIPS, 8, 128)
    )


def spread_body(p_ref, out_ref):
    core = lax.axis_index("c")
    lane = lax.broadcasted_iota(jnp.int32, (128, 256), 0)
    k = lax.broadcasted_iota(jnp.int32, (128, 256), 1)
    column = (lax.broadcasted_iota(jnp.int32, (16, 256), 1) >> 2) & 3
    for side in range(2):
        half = core if side == 0 else 1 - core
        pick = jnp.where(lane == (k >> 4) * 8 + half * 4 + (k & 3), 1.0, 0.0).astype(BF)
        for q in range(4):
            rows = jnp.dot(p_ref[q, 128:144, 0:128], pick, preferred_element_type=F32)
            for cb in range(4):
                out_ref[side, cb * 16 : cb * 16 + 16, q * 256 : q * 256 + 256] = jnp.where(
                    column == cb, rows, 0.0
                ).astype(BF)


def decay_update_body(
    got_ref, weight_ref, mean_ref, var_ref, new_out, copy_out, mean_out, var_out, rows
):
    dec = got_ref[:, 16:24, :].astype(F32)
    rows[...] = (dec + pltpu.roll(dec, 4, 1)).reshape(CHIPS * 8, 128)
    for b in range(D // 128):
        lanes = slice(b * 128, (b + 1) * 128)
        grad = rows[pl.ds((b // 4) * 8 + b % 4, H, stride=32), :]
        mean_new = 0.9 * mean_ref[:, lanes] + 0.1 * grad
        var_new = 0.95 * var_ref[:, lanes] + 0.05 * grad * grad
        new = weight_ref[:, lanes] - 0.5 * mean_new / (jnp.sqrt(var_new) + 1e-08)
        mean_out[:, lanes] = mean_new
        var_out[:, lanes] = var_new
        new_out[:, lanes] = new
        copy_out[:, lanes] = new.astype(BF)


def squares_body(near_ref, out_ref):
    near = near_ref[:, 0:16, :].astype(F32)
    sums = jnp.sum(near * near, axis=0)
    sums = sums[0:8] + sums[8:16]
    out_ref[...] = jnp.broadcast_to(sums[None], (8, 8, 128))


def product_body(rows_ref, near_ref, far_ref, out_ref):
    near = near_ref[:, 0:16, :].reshape(CHIPS * 16, 128)
    far = far_ref[:, 0:16, :].reshape(CHIPS * 16, 128)
    got = jnp.dot(rows_ref[0], near, preferred_element_type=F32) + jnp.dot(
        rows_ref[1], far, preferred_element_type=F32
    )
    for cb in range(4):
        out_ref[:, cb * 128 : cb * 128 + 128] = got[cb * 16 : cb * 16 + 16]


def step_body(squares_ref, delta_ref, weight_ref, step_out, new_out, copy_out):
    root_mean = jnp.sqrt(jnp.sum(squares_ref[...]) / (R * W) + 1e-06)
    step = -0.5 / root_mean * delta_ref[...]
    new = weight_ref[...] + step
    step_out[...] = step
    new_out[...] = new
    copy_out[...] = new.astype(BF)


def local(
    inputs,
    values_cot,
    decay_cot,
    factor,
    value_weight,
    lowrank_mean,
    lowrank_var,
    decay_weight,
    decay_mean,
    decay_var,
):
    chunk = shape((CHIPS, 24, 128), BF)
    near = lax.all_to_all(
        jnp.broadcast_to(factor, (CHIPS, 16, 128)), PLANE, 0, 0, tiled=True
    )
    decay_rows = call(
        decay_body,
        shape((CHIPS, 8, 128), BF),
        2,
        2 * 768 * D * H,
        4 << 20,
        [pltpu.VMEM((512, 128), F32)],
    )(decay_cot.T, inputs)
    near, decay_rows = lax.optimization_barrier((near, decay_rows))
    far = lax.ppermute(near, "c", SWAP)
    quarter = call(
        project_body,
        shape((144, 768), BF),
        4,
        2 * 768 * D * 128,
        4 << 20,
        [pltpu.VMEM((CHIPS, 2, 16, 128), BF)],
    )(inputs, near, far, factor)
    projected = lax.all_gather(quarter, "x")

    def gradient(half):
        return call(
            functools.partial(gradient_body, half),
            chunk,
            3,
            2 * 768 * 256 * 512,
            2 << 20,
            [pltpu.VMEM((CHIPS * 16, 128), F32)],
        )(projected, values_cot, decay_rows)

    peer = lax.ppermute(gradient(0), "c", SWAP)
    paired = call(pair_body, chunk, 2, 400000, 1 << 20)(gradient(1), peer)
    arrived = lax.all_to_all(paired, PLANE, 0, 0, tiled=True)
    rows = call(spread_body, shape((2, 64, 1024), BF), 1, 8 * 2 * 16 * 128 * 256, 1 << 20)(
        projected
    )
    ratio, mean_new, var_new = call(
        moment_body,
        (chunk, shape((4, 512), F32), shape((4, 512), F32)),
        3,
        400000,
        1 << 20,
        [pltpu.VMEM((16, 128), F32)] * 2,
    )(arrived, lowrank_mean, lowrank_var)
    near = lax.all_to_all(ratio, PLANE, 0, 0, tiled=True)
    far = lax.ppermute(near, "c", SWAP)
    state = shape((H, D), F32)
    decay_new, decay_copy, decay_mean_new, decay_var_new = call(
        decay_update_body,
        (state, shape((H, D), BF), state, state),
        4,
        400000,
        1 << 20,
        [pltpu.VMEM((512, 128), F32)],
    )(near, decay_weight.T, decay_mean.T, decay_var.T)
    squares = call(squares_body, shape((8, 8, 128), F32), 1, 400000, 1 << 20)(near)
    squares = lax.all_to_all(squares, ("c", "x"), 0, 0, tiled=True)
    delta = call(
        product_body, shape((16, 512), F32), 3, 2 * 64 * 2048 * 128, 1 << 20
    )(rows, near, far)
    block = shape((16, 512), F32)
    value_step, value_new, value_copy = call(
        step_body, (block, block, shape((16, 512), BF)), 3, 40000, 100000
    )(squares, delta, value_weight)
    return (
        value_step,
        value_new,
        value_copy,
        mean_new,
        var_new,
        decay_new.T,
        decay_copy.T,
        decay_mean_new.T,
        decay_var_new.T,
    )


def solution(mesh):
    split = Mesh(mesh.devices.reshape(8, 8, 2, mesh.shape["tp"]), ("z", "y", "c", "x"))
    placed = (
        P(FS, None),
        P(FS, "x"),
        P(FS, None),
        P(FS, "x"),
        P(FS, "x"),
        P(FS, "x"),
        P(FS, "x"),
        P(),
        P(),
        P(),
    )
    return jax.shard_map(
        local,
        mesh=split,
        in_specs=placed,
        out_specs=(P(FS, "x"),) * 5 + (P(),) * 4,
        check_vma=False,
    )
```

```python
import jax
import jax.numpy as jnp
from jax import lax
from jax.experimental import pallas as pl
from jax.experimental.pallas import tpu as pltpu
from jax.sharding import Mesh
from jax.sharding import PartitionSpec as P

D = 2048
W = 2048
R = 512
H = 16
FS = ("z", "y", "c")
PLANE = ("z", "y")
CHIPS = 64
SWAP = [(0, 1), (1, 0)]
BF = jnp.bfloat16
F32 = jnp.float32
VMEM = pl.BlockSpec(memory_space=pltpu.VMEM)


def call(body, outs, count, flops, moved, scratch=()):
    return pl.pallas_call(
        body,
        out_shape=outs,
        in_specs=[VMEM] * count,
        out_specs=jax.tree.map(lambda _: VMEM, outs),
        scratch_shapes=list(scratch),
        compiler_params=pltpu.CompilerParams(vmem_limit_bytes=12 << 20),
        cost_estimate=pl.CostEstimate(flops=flops, bytes_accessed=moved, transcendentals=0),
    )


def shape(dims, dtype):
    return jax.ShapeDtypeStruct(dims, dtype)


def split_pair(pair, axis):
    total = pair + pltpu.roll(pair, 4, axis)
    high = total.astype(BF).astype(F32)
    row = lax.broadcasted_iota(jnp.int32, pair.shape, axis)
    return jnp.where(row < 4, high, total - high)


def decay_body(cot_ref, x_ref, out_ref, rows):
    part = jnp.dot(cot_ref[...], x_ref[...], preferred_element_type=F32)
    high = part.astype(BF).astype(F32)
    low = part - high
    for b in range(D // 128):
        at = (b // 4) * 8 + b % 4
        lanes = slice(b * 128, (b + 1) * 128)
        rows[pl.ds(at, H, stride=32), :] = high[:, lanes]
        rows[pl.ds(at + 4, H, stride=32), :] = low[:, lanes]
    out_ref[...] = rows[...].astype(BF).reshape(CHIPS, 8, 128)


def pair_body(own_ref, peer_ref, out_ref):
    dec = own_ref[...].astype(F32) + peer_ref[...].astype(F32)
    out_ref[...] = split_pair(dec, 1).astype(BF)


def project_body(x_ref, near_ref, far_ref, own_ref, out_ref, whole):
    core = lax.axis_index("c")
    whole[:, pl.ds(core, 1)] = near_ref[...].reshape(CHIPS, 1, 16, 128)
    whole[:, pl.ds(1 - core, 1)] = far_ref[...].reshape(CHIPS, 1, 16, 128)
    part = jnp.dot(
        x_ref[...], whole[...].reshape(D, 128), preferred_element_type=F32
    ).astype(BF)
    a = lax.broadcasted_iota(jnp.int32, (128, 128), 0)
    lane = lax.broadcasted_iota(jnp.int32, (128, 128), 1)
    source = (a & 15) * 8 + (a >> 6) * 4 + ((a >> 4) & 3)
    order = jnp.where(lane == source, 1.0, 0.0).astype(BF)
    turned = lax.dot_general(
        order, part, (((1,), (1,)), ((), ())), preferred_element_type=F32
    ).astype(BF)
    for to in range(8):
        out_ref[to, 0:64, :] = turned[(to // 4) * 64 : (to // 4) * 64 + 64]
        out_ref[to, 64:72, :] = jnp.zeros((8, 768), BF)
        out_ref[to, 64:72, 0:128] = own_ref[0:8]
        out_ref[to, 64:72, 128:256] = own_ref[8:16]


def gradient_body(p_ref, own_ref, peer_ref, dec_ref, out_ref, rows):
    core = lax.axis_index("c")
    own = p_ref[pl.ds(core * 4, 4), 0:64, :].reshape(256, 768)
    peer = p_ref[pl.ds((1 - core) * 4, 4), 0:64, :].reshape(256, 768)
    part = jnp.dot(own, own_ref[...], preferred_element_type=F32) + jnp.dot(
        peer, peer_ref[...], preferred_element_type=F32
    )
    for q in range(4):
        for i in range(4):
            for cb in range(4):
                rows[pl.ds(q * 256 + cb * 4 + i, 16, stride=16), :] = part[
                    q * 64 + i * 16 : q * 64 + i * 16 + 16, cb * 128 : cb * 128 + 128
                ]
    out_ref[:, 0:16, :] = rows[...].astype(BF).reshape(CHIPS, 16, 128)
    out_ref[:, 16:24, :] = dec_ref[...]


def moment_body(got_ref, mean_ref, var_ref, out_ref, mean_out, var_out, mean_s, var_s):
    for cb in range(4):
        lanes = slice(cb * 128, cb * 128 + 128)
        mean_s[cb * 4 : cb * 4 + 4, :] = mean_ref[:, lanes]
        var_s[cb * 4 : cb * 4 + 4, :] = var_ref[:, lanes]
    grad = jnp.sum(got_ref[:, 0:16, :].astype(F32), axis=0)
    dec = jnp.sum(got_ref[:, 16:24, :].astype(F32), axis=0)
    mean_new = 0.9 * mean_s[...] + 0.1 * grad
    var_new = 0.95 * var_s[...] + 0.05 * grad * grad
    ratio = mean_new / (jnp.sqrt(var_new) + 1e-08)
    mean_s[...] = mean_new
    var_s[...] = var_new
    for cb in range(4):
        lanes = slice(cb * 128, cb * 128 + 128)
        mean_out[:, lanes] = mean_s[cb * 4 : cb * 4 + 4, :]
        var_out[:, lanes] = var_s[cb * 4 : cb * 4 + 4, :]
    out_ref[:, 0:16, :] = jnp.broadcast_to(ratio.astype(BF)[None], (CHIPS, 16, 128))
    out_ref[:, 16:24, :] = jnp.broadcast_to(
        split_pair(dec, 0).astype(BF)[None], (CHIPS, 8, 128)
    )


def spread_body(p_ref, out_ref):
    core = lax.axis_index("c")
    lane = lax.broadcasted_iota(jnp.int32, (128, 256), 0)
    k = lax.broadcasted_iota(jnp.int32, (128, 256), 1)
    column = (lax.broadcasted_iota(jnp.int32, (16, 256), 1) >> 2) & 3
    for side in range(2):
        half = core if side == 0 else 1 - core
        pick = jnp.where(lane == (k >> 4) * 8 + half * 4 + (k & 3), 1.0, 0.0).astype(BF)
        for q in range(4):
            own = jnp.concatenate(
                [
                    p_ref[core * 4 + q, 64:72, 0:128].astype(F32),
                    p_ref[core * 4 + q, 64:72, 128:256].astype(F32),
                ]
            ).astype(BF)
            rows = jnp.dot(own, pick, preferred_element_type=F32)
            for cb in range(4):
                out_ref[side, cb * 16 : cb * 16 + 16, q * 256 : q * 256 + 256] = jnp.where(
                    column == cb, rows, 0.0
                ).astype(BF)


def decay_update_body(
    got_ref, weight_ref, mean_ref, var_ref, new_out, copy_out, mean_out, var_out, rows
):
    dec = got_ref[:, 16:24, :].astype(F32)
    rows[...] = (dec + pltpu.roll(dec, 4, 1)).reshape(CHIPS * 8, 128)
    for b in range(D // 128):
        lanes = slice(b * 128, (b + 1) * 128)
        grad = rows[pl.ds((b // 4) * 8 + b % 4, H, stride=32), :]
        mean_new = 0.9 * mean_ref[:, lanes] + 0.1 * grad
        var_new = 0.95 * var_ref[:, lanes] + 0.05 * grad * grad
        new = weight_ref[:, lanes] - 0.5 * mean_new / (jnp.sqrt(var_new) + 1e-08)
        mean_out[:, lanes] = mean_new
        var_out[:, lanes] = var_new
        new_out[:, lanes] = new
        copy_out[:, lanes] = new.astype(BF)


def squares_body(near_ref, out_ref):
    near = near_ref[:, 0:16, :].astype(F32)
    sums = jnp.sum(near * near, axis=0)
    sums = sums[0:8] + sums[8:16]
    out_ref[...] = jnp.broadcast_to(sums[None], (8, 8, 128))


def product_body(rows_ref, near_ref, far_ref, out_ref):
    near = near_ref[:, 0:16, :].reshape(CHIPS * 16, 128)
    far = far_ref[:, 0:16, :].reshape(CHIPS * 16, 128)
    got = jnp.dot(rows_ref[0], near, preferred_element_type=F32) + jnp.dot(
        rows_ref[1], far, preferred_element_type=F32
    )
    for cb in range(4):
        out_ref[:, cb * 128 : cb * 128 + 128] = got[cb * 16 : cb * 16 + 16]


def step_body(squares_ref, delta_ref, weight_ref, step_out, new_out, copy_out):
    root_mean = jnp.sqrt(jnp.sum(squares_ref[...]) / (R * W) + 1e-06)
    step = -0.5 / root_mean * delta_ref[...]
    new = weight_ref[...] + step
    step_out[...] = step
    new_out[...] = new
    copy_out[...] = new.astype(BF)


def local(
    inputs,
    values_cot,
    decay_cot,
    factor,
    value_weight,
    lowrank_mean,
    lowrank_var,
    decay_weight,
    decay_mean,
    decay_var,
):
    chunk = shape((CHIPS, 24, 128), BF)
    near = lax.all_to_all(
        jnp.broadcast_to(factor, (CHIPS, 16, 128)), PLANE, 0, 0, tiled=True
    )
    decay_rows = call(
        decay_body,
        shape((CHIPS, 8, 128), BF),
        2,
        2 * 768 * D * H,
        4 << 20,
        [pltpu.VMEM((512, 128), F32)],
    )(decay_cot.T, inputs)
    values_peer = lax.ppermute(values_cot, "c", SWAP)
    decay_rows = call(pair_body, shape((CHIPS, 8, 128), BF), 2, 400000, 1 << 20)(
        decay_rows, lax.ppermute(decay_rows, "c", SWAP)
    )
    near, decay_rows, values_peer = lax.optimization_barrier((near, decay_rows, values_peer))
    far = lax.ppermute(near, "c", SWAP)
    parts = call(
        project_body,
        shape((8, 72, 768), BF),
        4,
        2 * 768 * D * 128,
        4 << 20,
        [pltpu.VMEM((CHIPS, 2, 16, 128), BF)],
    )(inputs, near, far, factor)
    projected = lax.all_to_all(parts, ("c", "x"), 0, 0, tiled=True)
    paired = call(
        gradient_body,
        chunk,
        4,
        2 * 1536 * 256 * 512,
        3 << 20,
        [pltpu.VMEM((CHIPS * 16, 128), F32)],
    )(projected, values_cot, values_peer, decay_rows)
    arrived = lax.all_to_all(paired, PLANE, 0, 0, tiled=True)
    rows = call(spread_body, shape((2, 64, 1024), BF), 1, 8 * 2 * 16 * 128 * 256, 1 << 20)(
        projected
    )
    ratio, mean_new, var_new = call(
        moment_body,
        (chunk, shape((4, 512), F32), shape((4, 512), F32)),
        3,
        400000,
        1 << 20,
        [pltpu.VMEM((16, 128), F32)] * 2,
    )(arrived, lowrank_mean, lowrank_var)
    near = lax.all_to_all(ratio, PLANE, 0, 0, tiled=True)
    far = lax.ppermute(near, "c", SWAP)
    state = shape((H, D), F32)
    decay_new, decay_copy, decay_mean_new, decay_var_new = call(
        decay_update_body,
        (state, shape((H, D), BF), state, state),
        4,
        400000,
        1 << 20,
        [pltpu.VMEM((512, 128), F32)],
    )(near, decay_weight.T, decay_mean.T, decay_var.T)
    squares = call(squares_body, shape((8, 8, 128), F32), 1, 400000, 1 << 20)(near)
    squares = lax.all_to_all(squares, ("c", "x"), 0, 0, tiled=True)
    delta = call(
        product_body, shape((16, 512), F32), 3, 2 * 64 * 2048 * 128, 1 << 20
    )(rows, near, far)
    block = shape((16, 512), F32)
    value_step, value_new, value_copy = call(
        step_body, (block, block, shape((16, 512), BF)), 3, 40000, 100000
    )(squares, delta, value_weight)
    return (
        value_step,
        value_new,
        value_copy,
        mean_new,
        var_new,
        decay_new.T,
        decay_copy.T,
        decay_mean_new.T,
        decay_var_new.T,
    )


def solution(mesh):
    split = Mesh(mesh.devices.reshape(8, 8, 2, mesh.shape["tp"]), ("z", "y", "c", "x"))
    placed = (
        P(FS, None),
        P(FS, "x"),
        P(FS, None),
        P(FS, "x"),
        P(FS, "x"),
        P(FS, "x"),
        P(FS, "x"),
        P(),
        P(),
        P(),
    )
    return jax.shard_map(
        local,
        mesh=split,
        in_specs=placed,
        out_specs=(P(FS, "x"),) * 5 + (P(),) * 4,
        check_vma=False,
    )
```

```python
import functools

import jax
import jax.numpy as jnp
from jax import lax
from jax.experimental import pallas as pl
from jax.experimental.pallas import tpu as pltpu
from jax.sharding import Mesh
from jax.sharding import PartitionSpec as P

D = 2048
W = 2048
R = 512
H = 16
FS = ("z", "y", "c")
PLANE = ("z", "y")
CHIPS = 64
CHUNK = 20
ROWS = CHIPS * CHUNK
SWAP = [(0, 1), (1, 0)]
BF = jnp.bfloat16
F32 = jnp.float32
VMEM = pl.BlockSpec(memory_space=pltpu.VMEM)


def call(body, outs, count, flops, moved, scratch=()):
    return pl.pallas_call(
        body,
        out_shape=outs,
        in_specs=[VMEM] * count,
        out_specs=jax.tree.map(lambda _: VMEM, outs),
        scratch_shapes=list(scratch),
        compiler_params=pltpu.CompilerParams(vmem_limit_bytes=12 << 20),
        cost_estimate=pl.CostEstimate(flops=flops, bytes_accessed=moved, transcendentals=0),
    )


def shape(dims, dtype):
    return jax.ShapeDtypeStruct(dims, dtype)


def decay_body(cot_ref, x_ref, out_ref):
    part = jnp.dot(cot_ref[...], x_ref[...], preferred_element_type=F32)
    high = part.astype(BF).astype(F32)
    low = part - high
    for b in range(D // 128):
        half, k = (b % 4) // 2, b % 2
        at = (b // 4) * 4 + k
        lanes = slice(b * 128, (b + 1) * 128)
        out_ref[half, pl.ds(at, H, stride=16), :] = high[:, lanes]
        out_ref[half, pl.ds(at + 2, H, stride=16), :] = low[:, lanes]


def project_body(x_ref, near_ref, far_ref, own_ref, out_ref, whole):
    core = lax.axis_index("c")
    whole[:, pl.ds(core, 1)] = near_ref[...].reshape(CHIPS, 1, 16, 128)
    whole[:, pl.ds(1 - core, 1)] = far_ref[...].reshape(CHIPS, 1, 16, 128)
    part = jnp.dot(
        x_ref[...], whole[...].reshape(D, 128), preferred_element_type=F32
    ).astype(BF)
    a = lax.broadcasted_iota(jnp.int32, (128, 128), 0)
    lane = lax.broadcasted_iota(jnp.int32, (128, 128), 1)
    half = jnp.where(a < 64, 1 - core, core)
    source = (a & 15) * 8 + half * 4 + ((a >> 4) & 3)
    order = jnp.where(lane == source, 1.0, 0.0).astype(BF)
    turned = lax.dot_general(
        order, part, (((1,), (1,)), ((), ())), preferred_element_type=F32
    ).astype(BF)
    out_ref[0:128, :] = turned
    out_ref[128:136, :] = jnp.zeros((8, 768), BF)
    out_ref[128:136, 0:128] = own_ref[0:8]
    out_ref[128:136, 128:256] = own_ref[8:16]


def gradient_body(half, p_ref, v_ref, dec_ref, out_ref, rows):
    core = lax.axis_index("c")
    for q in range(4):
        part = jnp.dot(
            p_ref[q, half * 64 : half * 64 + 64, :], v_ref[...], preferred_element_type=F32
        )
        for i in range(4):
            for cb in range(4):
                rows[pl.ds(q * 16 * CHUNK + cb * 4 + i, 16, stride=CHUNK), :] = part[
                    i * 16 : i * 16 + 16, cb * 128 : cb * 128 + 128
                ]
    side = core if half == 1 else 1 - core
    for k in range(4):
        rows[pl.ds(16 + k, CHIPS, stride=CHUNK), :] = dec_ref[
            side, pl.ds(k, CHIPS, stride=4), :
        ]
    out_ref[...] = rows[...].astype(BF)


def pair_body(own_ref, peer_ref, out_ref, rows):
    rows[...] = own_ref[...].astype(F32) + peer_ref[...].astype(F32)
    for k in range(2):
        at = pl.ds(16 + k, CHIPS, stride=CHUNK)
        below = pl.ds(18 + k, CHIPS, stride=CHUNK)
        total = rows[at, :] + rows[below, :]
        high = total.astype(BF).astype(F32)
        rows[at, :] = high
        rows[below, :] = total - high
    out_ref[...] = rows[...].astype(BF)


def moment_body(got_ref, mean_ref, var_ref, out_ref, mean_out, var_out, mean_s, var_s, sums, new):
    for cb in range(4):
        lanes = slice(cb * 128, cb * 128 + 128)
        mean_s[cb * 4 : cb * 4 + 4, :] = mean_ref[:, lanes]
        var_s[cb * 4 : cb * 4 + 4, :] = var_ref[:, lanes]
    sums[...] = jnp.sum(got_ref[...].astype(F32).reshape(CHIPS // 2, 2 * CHUNK, 128), axis=0)
    grad = sums[0:16, :] + sums[CHUNK : CHUNK + 16, :]
    dec = (
        sums[16:18, :]
        + sums[18:20, :]
        + sums[CHUNK + 16 : CHUNK + 18, :]
        + sums[CHUNK + 18 : CHUNK + 20, :]
    )
    mean_new = 0.9 * mean_s[...] + 0.1 * grad
    var_new = 0.95 * var_s[...] + 0.05 * grad * grad
    ratio = mean_new / (jnp.sqrt(var_new) + 1e-08)
    mean_s[...] = mean_new
    var_s[...] = var_new
    for cb in range(4):
        lanes = slice(cb * 128, cb * 128 + 128)
        mean_out[:, lanes] = mean_s[cb * 4 : cb * 4 + 4, :]
        var_out[:, lanes] = var_s[cb * 4 : cb * 4 + 4, :]
    high = dec.astype(BF).astype(F32)
    for copy in range(4):
        new[copy * CHUNK : copy * CHUNK + 16, :] = ratio
        new[copy * CHUNK + 16 : copy * CHUNK + 18, :] = high
        new[copy * CHUNK + 18 : copy * CHUNK + 20, :] = dec - high
    four = new[...].astype(BF)
    for at in range(0, ROWS, 4 * CHUNK):
        out_ref[at : at + 4 * CHUNK, :] = four


def spread_body(p_ref, out_ref):
    core = lax.axis_index("c")
    wide = 16 * CHUNK
    lane = lax.broadcasted_iota(jnp.int32, (128, wide), 0)
    k = lax.broadcasted_iota(jnp.int32, (128, wide), 1)
    chip = (k * 3277) >> 16
    row = k - chip * CHUNK
    mine = lax.broadcasted_iota(jnp.int32, (16, wide), 1)
    column = (mine - ((mine * 3277) >> 16) * CHUNK) >> 2
    for side in range(2):
        half = core if side == 0 else 1 - core
        hit = (lane == chip * 8 + half * 4 + (row & 3)) & (row < 16)
        pick = jnp.where(hit, 1.0, 0.0).astype(BF)
        for q in range(4):
            own = jnp.concatenate(
                [
                    p_ref[q, 128:136, 0:128].astype(F32),
                    p_ref[q, 128:136, 128:256].astype(F32),
                ]
            ).astype(BF)
            rows = jnp.dot(own, pick, preferred_element_type=F32)
            for cb in range(4):
                out_ref[side, q, cb * 16 : cb * 16 + 16, :] = jnp.where(
                    column == cb, rows, 0.0
                ).astype(BF)


def decay_update_body(
    near_ref, far_ref, weight_ref, mean_ref, var_ref, new_out, copy_out, mean_out, var_out, rows
):
    core = lax.axis_index("c")
    rows[core] = near_ref[...].astype(F32)
    rows[1 - core] = far_ref[...].astype(F32)
    for b in range(D // 128):
        half, k = (b % 4) // 2, b % 2
        at = (b // 4) * CHUNK + 16 + k
        lanes = slice(b * 128, (b + 1) * 128)
        grad = (
            rows[half, pl.ds(at, H, stride=4 * CHUNK), :]
            + rows[half, pl.ds(at + 2, H, stride=4 * CHUNK), :]
        )
        mean_new = 0.9 * mean_ref[:, lanes] + 0.1 * grad
        var_new = 0.95 * var_ref[:, lanes] + 0.05 * grad * grad
        new = weight_ref[:, lanes] - 0.5 * mean_new / (jnp.sqrt(var_new) + 1e-08)
        mean_out[:, lanes] = mean_new
        var_out[:, lanes] = var_new
        new_out[:, lanes] = new
        copy_out[:, lanes] = new.astype(BF)


def squares_body(near_ref, out_ref):
    near = near_ref[...].astype(F32).reshape(CHIPS // 4, 4 * CHUNK, 128)
    row = lax.broadcasted_iota(jnp.int32, (4 * CHUNK, 128), 0)
    row = row - ((row * 3277) >> 16) * CHUNK
    sums = jnp.where(row < 16, jnp.sum(near * near, axis=0), 0.0)
    sums = jnp.sum(sums.reshape(CHUNK // 2, 8, 128), axis=0)
    out_ref[...] = jnp.broadcast_to(sums[None], (8, 8, 128))


def product_body(rows_ref, near_ref, far_ref, out_ref):
    got = jnp.zeros((64, 128), F32)
    for q in range(4):
        part = slice(q * 16 * CHUNK, (q + 1) * 16 * CHUNK)
        got += jnp.dot(rows_ref[0, q], near_ref[part, :], preferred_element_type=F32)
        got += jnp.dot(rows_ref[1, q], far_ref[part, :], preferred_element_type=F32)
    for cb in range(4):
        out_ref[:, cb * 128 : cb * 128 + 128] = got[cb * 16 : cb * 16 + 16]


def step_body(squares_ref, delta_ref, weight_ref, step_out, new_out, copy_out):
    root_mean = jnp.sqrt(jnp.sum(squares_ref[...]) / (R * W) + 1e-06)
    step = -0.5 / root_mean * delta_ref[...]
    new = weight_ref[...] + step
    step_out[...] = step
    new_out[...] = new
    copy_out[...] = new.astype(BF)


def local(
    inputs,
    values_cot,
    decay_cot,
    factor,
    value_weight,
    lowrank_mean,
    lowrank_var,
    decay_weight,
    decay_mean,
    decay_var,
):
    chunk = shape((ROWS, 128), BF)

    def across(rows):
        tiles = rows.reshape(CHIPS, CHUNK // 4, 4, 128)
        return lax.all_to_all(tiles, PLANE, 0, 0, tiled=True).reshape(ROWS, 128)

    near = lax.all_to_all(
        jnp.broadcast_to(factor, (CHIPS, 16, 128)), PLANE, 0, 0, tiled=True
    )
    decay_rows = call(
        decay_body,
        shape((2, CHIPS * 4, 128), F32),
        2,
        2 * 768 * D * H,
        4 << 20,
    )(decay_cot.T, inputs)
    near, decay_rows = lax.optimization_barrier((near, decay_rows))
    far = lax.ppermute(near, "c", SWAP)
    quarter = call(
        project_body,
        shape((136, 768), BF),
        4,
        2 * 768 * D * 128,
        4 << 20,
        [pltpu.VMEM((CHIPS, 2, 16, 128), BF)],
    )(inputs, near, far, factor)
    projected = lax.all_gather(quarter, "x")

    def gradient(half):
        return call(
            functools.partial(gradient_body, half),
            chunk,
            3,
            2 * 768 * 256 * 512,
            2 << 20,
            [pltpu.VMEM((ROWS, 128), F32)],
        )(projected, values_cot, decay_rows)

    peer = lax.ppermute(gradient(0), "c", SWAP)
    paired = call(
        pair_body, chunk, 2, 400000, 1 << 20, [pltpu.VMEM((ROWS, 128), F32)]
    )(gradient(1), peer)
    arrived = across(paired)
    rows = call(spread_body, shape((2, 4, 64, 16 * CHUNK), BF), 1, 8 * 2 * 16 * 128 * 256, 1 << 20)(
        projected
    )
    ratio, mean_new, var_new = call(
        moment_body,
        (chunk, shape((4, 512), F32), shape((4, 512), F32)),
        3,
        400000,
        1 << 20,
        [
            pltpu.VMEM((16, 128), F32),
            pltpu.VMEM((16, 128), F32),
            pltpu.VMEM((2 * CHUNK, 128), F32),
            pltpu.VMEM((4 * CHUNK, 128), F32),
        ],
    )(arrived, lowrank_mean, lowrank_var)
    near = across(ratio)
    far = lax.ppermute(near, "c", SWAP)
    state = shape((H, D), F32)
    decay_new, decay_copy, decay_mean_new, decay_var_new = call(
        decay_update_body,
        (state, shape((H, D), BF), state, state),
        5,
        400000,
        1 << 20,
        [pltpu.VMEM((2, ROWS, 128), F32)],
    )(near, far, decay_weight.T, decay_mean.T, decay_var.T)
    squares = call(squares_body, shape((8, 8, 128), F32), 1, 400000, 1 << 20)(near)
    squares = lax.all_to_all(squares, ("c", "x"), 0, 0, tiled=True)
    delta = call(
        product_body, shape((16, 512), F32), 3, 2 * 64 * 2048 * 128, 1 << 20
    )(rows, near, far)
    block = shape((16, 512), F32)
    value_step, value_new, value_copy = call(
        step_body, (block, block, shape((16, 512), BF)), 3, 40000, 100000
    )(squares, delta, value_weight)
    return (
        value_step,
        value_new,
        value_copy,
        mean_new,
        var_new,
        decay_new.T,
        decay_copy.T,
        decay_mean_new.T,
        decay_var_new.T,
    )


def solution(mesh):
    split = Mesh(mesh.devices.reshape(8, 8, 2, mesh.shape["tp"]), ("z", "y", "c", "x"))
    placed = (
        P(FS, None),
        P(FS, "x"),
        P(FS, None),
        P(FS, "x"),
        P(FS, "x"),
        P(FS, "x"),
        P(FS, "x"),
        P(),
        P(),
        P(),
    )
    return jax.shard_map(
        local,
        mesh=split,
        in_specs=placed,
        out_specs=(P(FS, "x"),) * 5 + (P(),) * 4,
        check_vma=False,
    )
```

```python
import functools

import jax
import jax.numpy as jnp
from jax import lax
from jax.experimental import pallas as pl
from jax.experimental.pallas import tpu as pltpu
from jax.sharding import Mesh
from jax.sharding import PartitionSpec as P

D = 2048
W = 2048
R = 512
H = 16
FS = ("z", "y", "c")
PLANE = ("z", "y")
CHIPS = 64
CHUNK = 18
ROWS = CHIPS * CHUNK
SWAP = [(0, 1), (1, 0)]
BF = jnp.bfloat16
F32 = jnp.float32
VMEM = pl.BlockSpec(memory_space=pltpu.VMEM)


def call(body, outs, count, flops, moved, scratch=()):
    return pl.pallas_call(
        body,
        out_shape=outs,
        in_specs=[VMEM] * count,
        out_specs=jax.tree.map(lambda _: VMEM, outs),
        scratch_shapes=list(scratch),
        compiler_params=pltpu.CompilerParams(vmem_limit_bytes=12 << 20),
        cost_estimate=pl.CostEstimate(flops=flops, bytes_accessed=moved, transcendentals=0),
    )


def shape(dims, dtype):
    return jax.ShapeDtypeStruct(dims, dtype)


def decay_body(cot_ref, x_ref, out_ref, rows):
    part = jnp.dot(cot_ref[...], x_ref[...], preferred_element_type=F32)
    for b in range(D // 128):
        half, at = (b % 4) // 2, (b // 4) * 2 + b % 2
        rows[half, pl.ds(at, H, stride=8), :] = part[:, b * 128 : (b + 1) * 128]
    out_ref[...] = rows[...].astype(BF)


def project_body(x_ref, near_ref, far_ref, own_ref, out_ref, whole):
    core = lax.axis_index("c")
    whole[:, pl.ds(core, 1)] = near_ref[...].reshape(CHIPS, 1, 16, 128)
    whole[:, pl.ds(1 - core, 1)] = far_ref[...].reshape(CHIPS, 1, 16, 128)
    part = jnp.dot(
        x_ref[...], whole[...].reshape(D, 128), preferred_element_type=F32
    ).astype(BF)
    a = lax.broadcasted_iota(jnp.int32, (128, 128), 0)
    lane = lax.broadcasted_iota(jnp.int32, (128, 128), 1)
    half = jnp.where(a < 64, 1 - core, core)
    source = (a & 15) * 8 + half * 4 + ((a >> 4) & 3)
    order = jnp.where(lane == source, 1.0, 0.0).astype(BF)
    turned = lax.dot_general(
        order, part, (((1,), (1,)), ((), ())), preferred_element_type=F32
    ).astype(BF)
    out_ref[0:128, :] = turned
    out_ref[128:144, :] = jnp.zeros((16, 768), BF)
    out_ref[128:144, 0:128] = own_ref[...]


def gradient_body(half, p_ref, v_ref, dec_ref, out_ref, rows, dec):
    core = lax.axis_index("c")
    for q in range(4):
        part = jnp.dot(
            p_ref[q, half * 64 : half * 64 + 64, :], v_ref[...], preferred_element_type=F32
        )
        for i in range(4):
            for cb in range(4):
                rows[pl.ds(q * 16 * CHUNK + cb * 4 + i, 16, stride=CHUNK), :] = part[
                    i * 16 : i * 16 + 16, cb * 128 : cb * 128 + 128
                ]
    side = core if half == 1 else 1 - core
    dec[...] = dec_ref[side].astype(F32)
    for k in range(2):
        rows[pl.ds(16 + k, CHIPS, stride=CHUNK), :] = dec[pl.ds(k, CHIPS, stride=2), :]
    out_ref[...] = rows[...].astype(BF)


def copies_body(own_ref, out_ref):
    out_ref[...] = jnp.broadcast_to(own_ref[...][None], (CHIPS, 16, 128))


def pair_body(own_ref, peer_ref, out_ref):
    out_ref[...] = (own_ref[...].astype(F32) + peer_ref[...].astype(F32)).astype(BF)


def moment_body(got_ref, mean_ref, var_ref, out_ref, mean_out, var_out, mean_s, var_s, sums, new):
    for cb in range(4):
        lanes = slice(cb * 128, cb * 128 + 128)
        mean_s[cb * 4 : cb * 4 + 4, :] = mean_ref[:, lanes]
        var_s[cb * 4 : cb * 4 + 4, :] = var_ref[:, lanes]
    sums[...] = jnp.sum(got_ref[...].astype(F32).reshape(CHIPS // 4, 4 * CHUNK, 128), axis=0)
    total = (
        sums[0:CHUNK, :]
        + sums[CHUNK : 2 * CHUNK, :]
        + sums[2 * CHUNK : 3 * CHUNK, :]
        + sums[3 * CHUNK : 4 * CHUNK, :]
    )
    grad = total[0:16]
    mean_new = 0.9 * mean_s[...] + 0.1 * grad
    var_new = 0.95 * var_s[...] + 0.05 * grad * grad
    ratio = mean_new / (jnp.sqrt(var_new) + 1e-08)
    mean_s[...] = mean_new
    var_s[...] = var_new
    for cb in range(4):
        lanes = slice(cb * 128, cb * 128 + 128)
        mean_out[:, lanes] = mean_s[cb * 4 : cb * 4 + 4, :]
        var_out[:, lanes] = var_s[cb * 4 : cb * 4 + 4, :]
    for copy in range(8):
        new[copy * CHUNK : copy * CHUNK + 16, :] = ratio
        new[copy * CHUNK + 16 : copy * CHUNK + 18, :] = total[16:18]
    eight = new[...].astype(BF)
    for at in range(0, ROWS, 8 * CHUNK):
        out_ref[at : at + 8 * CHUNK, :] = eight


def spread_body(p_ref, out_ref):
    core = lax.axis_index("c")
    wide = 16 * CHUNK
    lane = lax.broadcasted_iota(jnp.int32, (128, wide), 0)
    k = lax.broadcasted_iota(jnp.int32, (128, wide), 1)
    chip = (k * 3641) >> 16
    row = k - chip * CHUNK
    mine = lax.broadcasted_iota(jnp.int32, (16, wide), 1)
    column = (mine - ((mine * 3641) >> 16) * CHUNK) >> 2
    for side in range(2):
        half = core if side == 0 else 1 - core
        hit = (lane == chip * 8 + half * 4 + (row & 3)) & (row < 16)
        pick = jnp.where(hit, 1.0, 0.0).astype(BF)
        for q in range(4):
            rows = jnp.dot(p_ref[q, 128:144, 0:128], pick, preferred_element_type=F32)
            for cb in range(4):
                out_ref[side, q, cb * 16 : cb * 16 + 16, :] = jnp.where(
                    column == cb, rows, 0.0
                ).astype(BF)


def decay_update_body(
    near_ref, far_ref, weight_ref, mean_ref, var_ref, new_out, copy_out, mean_out, var_out, rows
):
    core = lax.axis_index("c")
    rows[core] = near_ref[...].astype(F32)
    rows[1 - core] = far_ref[...].astype(F32)
    for b in range(D // 128):
        half, k = (b % 4) // 2, b % 2
        at = (b // 4) * CHUNK + 16 + k
        lanes = slice(b * 128, (b + 1) * 128)
        grad = rows[half, pl.ds(at, H, stride=4 * CHUNK), :]
        mean_new = 0.9 * mean_ref[:, lanes] + 0.1 * grad
        var_new = 0.95 * var_ref[:, lanes] + 0.05 * grad * grad
        new = weight_ref[:, lanes] - 0.5 * mean_new / (jnp.sqrt(var_new) + 1e-08)
        mean_out[:, lanes] = mean_new
        var_out[:, lanes] = var_new
        new_out[:, lanes] = new
        copy_out[:, lanes] = new.astype(BF)


def squares_body(near_ref, out_ref):
    near = near_ref[...].astype(F32).reshape(CHIPS // 4, 4 * CHUNK, 128)
    row = lax.broadcasted_iota(jnp.int32, (4 * CHUNK, 128), 0)
    row = row - ((row * 3641) >> 16) * CHUNK
    sums = jnp.where(row < 16, jnp.sum(near * near, axis=0), 0.0)
    sums = jnp.sum(sums.reshape(4 * CHUNK // 8, 8, 128), axis=0)
    out_ref[...] = jnp.broadcast_to(sums[None], (8, 8, 128))


def product_body(rows_ref, near_ref, far_ref, out_ref):
    got = jnp.zeros((64, 128), F32)
    for q in range(4):
        part = slice(q * 16 * CHUNK, (q + 1) * 16 * CHUNK)
        got += jnp.dot(rows_ref[0, q], near_ref[part, :], preferred_element_type=F32)
        got += jnp.dot(rows_ref[1, q], far_ref[part, :], preferred_element_type=F32)
    for cb in range(4):
        out_ref[:, cb * 128 : cb * 128 + 128] = got[cb * 16 : cb * 16 + 16]


def step_body(squares_ref, delta_ref, weight_ref, step_out, new_out, copy_out):
    root_mean = jnp.sqrt(jnp.sum(squares_ref[...]) / (R * W) + 1e-06)
    step = -0.5 / root_mean * delta_ref[...]
    new = weight_ref[...] + step
    step_out[...] = step
    new_out[...] = new
    copy_out[...] = new.astype(BF)


def local(
    inputs,
    values_cot,
    decay_cot,
    factor,
    value_weight,
    lowrank_mean,
    lowrank_var,
    decay_weight,
    decay_mean,
    decay_var,
):
    chunk = shape((ROWS, 128), BF)

    def across(rows):
        tiles = rows.reshape(CHIPS, CHUNK // 2, 2, 128)
        return lax.all_to_all(tiles, PLANE, 0, 0, tiled=True).reshape(ROWS, 128)

    copies = call(copies_body, shape((CHIPS, 16, 128), BF), 1, 0, 1 << 18)(factor)
    near = lax.all_to_all(copies, PLANE, 0, 0, tiled=True)
    decay_rows = call(
        decay_body,
        shape((2, CHIPS * 2, 128), BF),
        2,
        2 * 768 * D * H,
        4 << 20,
        [pltpu.VMEM((2, CHIPS * 2, 128), F32)],
    )(decay_cot.T, inputs)
    near, decay_rows = lax.optimization_barrier((near, decay_rows))
    far = lax.ppermute(near, "c", SWAP)
    quarter = call(
        project_body,
        shape((144, 768), BF),
        4,
        2 * 768 * D * 128,
        4 << 20,
        [pltpu.VMEM((CHIPS, 2, 16, 128), BF)],
    )(inputs, near, far, factor)
    projected = lax.all_gather(quarter, "x")

    def gradient(half):
        return call(
            functools.partial(gradient_body, half),
            chunk,
            3,
            2 * 768 * 256 * 512,
            2 << 20,
            [pltpu.VMEM((ROWS, 128), F32), pltpu.VMEM((CHIPS * 2, 128), F32)],
        )(projected, values_cot, decay_rows)

    peer = lax.ppermute(gradient(0), "c", SWAP)
    paired = call(pair_body, chunk, 2, 400000, 1 << 20)(gradient(1), peer)
    arrived = across(paired)
    rows = call(spread_body, shape((2, 4, 64, 16 * CHUNK), BF), 1, 8 * 2 * 16 * 128 * 256, 1 << 20)(
        projected
    )
    ratio, mean_new, var_new = call(
        moment_body,
        (chunk, shape((4, 512), F32), shape((4, 512), F32)),
        3,
        400000,
        1 << 20,
        [
            pltpu.VMEM((16, 128), F32),
            pltpu.VMEM((16, 128), F32),
            pltpu.VMEM((4 * CHUNK, 128), F32),
            pltpu.VMEM((8 * CHUNK, 128), F32),
        ],
    )(arrived, lowrank_mean, lowrank_var)
    near = across(ratio)
    far = lax.ppermute(near, "c", SWAP)
    state = shape((H, D), F32)
    decay_new, decay_copy, decay_mean_new, decay_var_new = call(
        decay_update_body,
        (state, shape((H, D), BF), state, state),
        5,
        400000,
        1 << 20,
        [pltpu.VMEM((2, ROWS, 128), F32)],
    )(near, far, decay_weight.T, decay_mean.T, decay_var.T)
    squares = call(squares_body, shape((8, 8, 128), F32), 1, 400000, 1 << 20)(near)
    squares = lax.all_to_all(squares, ("c", "x"), 0, 0, tiled=True)
    delta = call(
        product_body, shape((16, 512), F32), 3, 2 * 64 * 2048 * 128, 1 << 20
    )(rows, near, far)
    block = shape((16, 512), F32)
    value_step, value_new, value_copy = call(
        step_body, (block, block, shape((16, 512), BF)), 3, 40000, 100000
    )(squares, delta, value_weight)
    return (
        value_step,
        value_new,
        value_copy,
        mean_new,
        var_new,
        decay_new.T,
        decay_copy.T,
        decay_mean_new.T,
        decay_var_new.T,
    )


def solution(mesh):
    split = Mesh(mesh.devices.reshape(8, 8, 2, mesh.shape["tp"]), ("z", "y", "c", "x"))
    placed = (
        P(FS, None),
        P(FS, "x"),
        P(FS, None),
        P(FS, "x"),
        P(FS, "x"),
        P(FS, "x"),
        P(FS, "x"),
        P(),
        P(),
        P(),
    )
    return jax.shard_map(
        local,
        mesh=split,
        in_specs=placed,
        out_specs=(P(FS, "x"),) * 5 + (P(),) * 4,
        check_vma=False,
    )
```

```python
import functools

import jax
import jax.numpy as jnp
from jax import lax
from jax.experimental import pallas as pl
from jax.experimental.pallas import tpu as pltpu
from jax.sharding import Mesh
from jax.sharding import PartitionSpec as P

D = 2048
W = 2048
R = 512
H = 16
FS = ("z", "y", "c")
PLANE = ("z", "y")
CHIPS = 64
CHUNK = 18
ROWS = CHIPS * CHUNK
SWAP = [(0, 1), (1, 0)]
BF = jnp.bfloat16
F32 = jnp.float32
VMEM = pl.BlockSpec(memory_space=pltpu.VMEM)


def call(body, outs, count, flops, moved, scratch=()):
    return pl.pallas_call(
        body,
        out_shape=outs,
        in_specs=[VMEM] * count,
        out_specs=jax.tree.map(lambda _: VMEM, outs),
        scratch_shapes=list(scratch),
        compiler_params=pltpu.CompilerParams(vmem_limit_bytes=12 << 20),
        cost_estimate=pl.CostEstimate(flops=flops, bytes_accessed=moved, transcendentals=0),
    )


def shape(dims, dtype):
    return jax.ShapeDtypeStruct(dims, dtype)


def decay_body(cot_ref, x_ref, out_ref, rows):
    part = jnp.dot(cot_ref[...], x_ref[...], preferred_element_type=F32)
    for b in range(D // 128):
        half, at = (b % 4) // 2, (b // 4) * 2 + b % 2
        rows[half, pl.ds(at, H, stride=8), :] = part[:, b * 128 : (b + 1) * 128]
    out_ref[...] = rows[...].astype(BF)


def project_body(x_ref, near_ref, far_ref, own_ref, out_ref, whole):
    core = lax.axis_index("c")
    whole[:, pl.ds(core, 1)] = near_ref[...].reshape(CHIPS, 1, 16, 128)
    whole[:, pl.ds(1 - core, 1)] = far_ref[...].reshape(CHIPS, 1, 16, 128)
    part = jnp.dot(
        x_ref[...], whole[...].reshape(D, 128), preferred_element_type=F32
    ).astype(BF)
    a = lax.broadcasted_iota(jnp.int32, (128, 128), 0)
    lane = lax.broadcasted_iota(jnp.int32, (128, 128), 1)
    half = jnp.where(a < 64, 1 - core, core)
    source = (a & 15) * 8 + half * 4 + ((a >> 4) & 3)
    order = jnp.where(lane == source, 1.0, 0.0).astype(BF)
    turned = lax.dot_general(
        order, part, (((1,), (1,)), ((), ())), preferred_element_type=F32
    ).astype(BF)
    out_ref[0:128, :] = turned
    out_ref[128:144, :] = jnp.zeros((16, 768), BF)
    out_ref[128:144, 0:128] = own_ref[...]


def gradient_body(half, p_ref, v_ref, dec_ref, out_ref, rows, dec):
    core = lax.axis_index("c")
    for q in range(4):
        part = jnp.dot(
            p_ref[q, half * 64 : half * 64 + 64, :], v_ref[...], preferred_element_type=F32
        )
        for i in range(4):
            for cb in range(4):
                rows[pl.ds(q * 16 * CHUNK + cb * 4 + i, 16, stride=CHUNK), :] = part[
                    i * 16 : i * 16 + 16, cb * 128 : cb * 128 + 128
                ]
    side = core if half == 1 else 1 - core
    dec[...] = dec_ref[side].astype(F32)
    for k in range(2):
        rows[pl.ds(16 + k, CHIPS, stride=CHUNK), :] = dec[pl.ds(k, CHIPS, stride=2), :]
    out_ref[...] = rows[...].astype(BF)


def copies_body(own_ref, out_ref):
    out_ref[...] = jnp.broadcast_to(own_ref[...][None], (CHIPS, 16, 128))


def pair_body(own_ref, peer_ref, out_ref):
    out_ref[...] = (own_ref[...].astype(F32) + peer_ref[...].astype(F32)).astype(BF)


def moment_body(got_ref, mean_ref, var_ref, out_ref, mean_out, var_out, mean_s, var_s, sums, new):
    for cb in range(4):
        lanes = slice(cb * 128, cb * 128 + 128)
        mean_s[cb * 4 : cb * 4 + 4, :] = mean_ref[:, lanes]
        var_s[cb * 4 : cb * 4 + 4, :] = var_ref[:, lanes]
    sums[...] = jnp.sum(got_ref[...].astype(F32).reshape(CHIPS // 4, 4 * CHUNK, 128), axis=0)
    total = (
        sums[0:CHUNK, :]
        + sums[CHUNK : 2 * CHUNK, :]
        + sums[2 * CHUNK : 3 * CHUNK, :]
        + sums[3 * CHUNK : 4 * CHUNK, :]
    )
    grad = total[0:16]
    mean_new = 0.9 * mean_s[...] + 0.1 * grad
    var_new = 0.95 * var_s[...] + 0.05 * grad * grad
    ratio = mean_new / (jnp.sqrt(var_new) + 1e-08)
    mean_s[...] = mean_new
    var_s[...] = var_new
    for cb in range(4):
        lanes = slice(cb * 128, cb * 128 + 128)
        mean_out[:, lanes] = mean_s[cb * 4 : cb * 4 + 4, :]
        var_out[:, lanes] = var_s[cb * 4 : cb * 4 + 4, :]
    for copy in range(8):
        new[copy * CHUNK : copy * CHUNK + 16, :] = ratio
        new[copy * CHUNK + 16 : copy * CHUNK + 18, :] = total[16:18]
    eight = new[...].astype(BF)
    for at in range(0, ROWS, 8 * CHUNK):
        out_ref[at : at + 8 * CHUNK, :] = eight


def spread_body(p_ref, out_ref):
    core = lax.axis_index("c")
    wide = 16 * CHUNK
    lane = lax.broadcasted_iota(jnp.int32, (128, wide), 0)
    k = lax.broadcasted_iota(jnp.int32, (128, wide), 1)
    chip = (k * 3641) >> 16
    row = k - chip * CHUNK
    mine = lax.broadcasted_iota(jnp.int32, (16, wide), 1)
    column = (mine - ((mine * 3641) >> 16) * CHUNK) >> 2
    for side in range(2):
        half = core if side == 0 else 1 - core
        hit = (lane == chip * 8 + half * 4 + (row & 3)) & (row < 16)
        pick = jnp.where(hit, 1.0, 0.0).astype(BF)
        for q in range(4):
            rows = jnp.dot(p_ref[q, 128:144, 0:128], pick, preferred_element_type=F32)
            for cb in range(4):
                out_ref[side, q, cb * 16 : cb * 16 + 16, :] = jnp.where(
                    column == cb, rows, 0.0
                ).astype(BF)


def decay_update_body(
    near_ref,
    far_ref,
    weight_ref,
    mean_ref,
    var_ref,
    low_mean_ref,
    low_var_ref,
    new_out,
    copy_out,
    mean_out,
    var_out,
    low_mean_out,
    low_var_out,
    rows,
):
    low_mean_out[...] = low_mean_ref[...]
    low_var_out[...] = low_var_ref[...]
    core = lax.axis_index("c")
    rows[core] = near_ref[...].astype(F32)
    rows[1 - core] = far_ref[...].astype(F32)
    for b in range(D // 128):
        half, k = (b % 4) // 2, b % 2
        at = (b // 4) * CHUNK + 16 + k
        lanes = slice(b * 128, (b + 1) * 128)
        grad = rows[half, pl.ds(at, H, stride=4 * CHUNK), :]
        mean_new = 0.9 * mean_ref[:, lanes] + 0.1 * grad
        var_new = 0.95 * var_ref[:, lanes] + 0.05 * grad * grad
        new = weight_ref[:, lanes] - 0.5 * mean_new / (jnp.sqrt(var_new) + 1e-08)
        mean_out[:, lanes] = mean_new
        var_out[:, lanes] = var_new
        new_out[:, lanes] = new
        copy_out[:, lanes] = new.astype(BF)


def squares_body(near_ref, out_ref):
    near = near_ref[...].astype(F32).reshape(CHIPS // 4, 4 * CHUNK, 128)
    row = lax.broadcasted_iota(jnp.int32, (4 * CHUNK, 128), 0)
    row = row - ((row * 3641) >> 16) * CHUNK
    sums = jnp.where(row < 16, jnp.sum(near * near, axis=0), 0.0)
    sums = jnp.sum(sums, axis=0, keepdims=True)
    out_ref[...] = jnp.broadcast_to(sums[None], (8, 1, 128))


def product_body(rows_ref, near_ref, far_ref, out_ref):
    got = jnp.zeros((64, 128), F32)
    for q in range(4):
        part = slice(q * 16 * CHUNK, (q + 1) * 16 * CHUNK)
        got += jnp.dot(rows_ref[0, q], near_ref[part, :], preferred_element_type=F32)
        got += jnp.dot(rows_ref[1, q], far_ref[part, :], preferred_element_type=F32)
    for cb in range(4):
        out_ref[:, cb * 128 : cb * 128 + 128] = got[cb * 16 : cb * 16 + 16]


def step_body(squares_ref, delta_ref, weight_ref, step_out, new_out, copy_out):
    root_mean = jnp.sqrt(jnp.sum(squares_ref[...]) / (R * W) + 1e-06)
    step = -0.5 / root_mean * delta_ref[...]
    new = weight_ref[...] + step
    step_out[...] = step
    new_out[...] = new
    copy_out[...] = new.astype(BF)


def local(
    inputs,
    values_cot,
    decay_cot,
    factor,
    value_weight,
    lowrank_mean,
    lowrank_var,
    decay_weight,
    decay_mean,
    decay_var,
):
    chunk = shape((ROWS, 128), BF)

    def across(rows):
        tiles = rows.reshape(CHIPS, CHUNK // 2, 2, 128)
        return lax.all_to_all(tiles, PLANE, 0, 0, tiled=True).reshape(ROWS, 128)

    copies = call(copies_body, shape((CHIPS, 16, 128), BF), 1, 0, 1 << 18)(factor)
    near = lax.all_to_all(copies, PLANE, 0, 0, tiled=True)
    decay_rows = call(
        decay_body,
        shape((2, CHIPS * 2, 128), BF),
        2,
        2 * 768 * D * H,
        4 << 20,
        [pltpu.VMEM((2, CHIPS * 2, 128), F32)],
    )(decay_cot.T, inputs)
    near, decay_rows = lax.optimization_barrier((near, decay_rows))
    far = lax.ppermute(near, "c", SWAP)
    quarter = call(
        project_body,
        shape((144, 768), BF),
        4,
        2 * 768 * D * 128,
        4 << 20,
        [pltpu.VMEM((CHIPS, 2, 16, 128), BF)],
    )(inputs, near, far, factor)
    projected = lax.all_gather(quarter, "x")

    def gradient(half):
        return call(
            functools.partial(gradient_body, half),
            chunk,
            3,
            2 * 768 * 256 * 512,
            2 << 20,
            [pltpu.VMEM((ROWS, 128), F32), pltpu.VMEM((CHIPS * 2, 128), F32)],
        )(projected, values_cot, decay_rows)

    theirs = gradient(0)
    peer = lax.ppermute(theirs, "c", SWAP)
    paired = call(pair_body, chunk, 2, 400000, 1 << 20)(gradient(1), peer)
    arrived = across(paired)
    rows = call(spread_body, shape((2, 4, 64, 16 * CHUNK), BF), 1, 8 * 2 * 16 * 128 * 256, 1 << 20)(
        projected
    )
    ratio, mean_new, var_new = call(
        moment_body,
        (chunk, pltpu.VMEM((4, 512), F32), pltpu.VMEM((4, 512), F32)),
        3,
        400000,
        1 << 20,
        [
            pltpu.VMEM((16, 128), F32),
            pltpu.VMEM((16, 128), F32),
            pltpu.VMEM((4 * CHUNK, 128), F32),
            pltpu.VMEM((8 * CHUNK, 128), F32),
        ],
    )(arrived, lowrank_mean, lowrank_var)
    near = across(ratio)
    far = lax.ppermute(near, "c", SWAP)
    state = shape((H, D), F32)
    low = shape((4, 512), F32)
    (decay_new, decay_copy, decay_mean_new, decay_var_new, mean_new, var_new) = call(
        decay_update_body,
        (state, shape((H, D), BF), state, state, low, low),
        7,
        400000,
        1 << 20,
        [pltpu.VMEM((2, ROWS, 128), F32)],
    )(near, far, decay_weight.T, decay_mean.T, decay_var.T, mean_new, var_new)
    squares = call(squares_body, shape((8, 1, 128), F32), 1, 400000, 1 << 20)(near)
    squares = lax.all_to_all(squares, ("c", "x"), 0, 0, tiled=True)
    delta = call(
        product_body, shape((16, 512), F32), 3, 2 * 64 * 2048 * 128, 1 << 20
    )(rows, near, far)
    block = shape((16, 512), F32)
    value_step, value_new, value_copy = call(
        step_body, (block, block, shape((16, 512), BF)), 3, 40000, 100000
    )(squares, delta, value_weight)
    return (
        value_step,
        value_new,
        value_copy,
        mean_new,
        var_new,
        decay_new.T,
        decay_copy.T,
        decay_mean_new.T,
        decay_var_new.T,
    )


def solution(mesh):
    split = Mesh(mesh.devices.reshape(8, 8, 2, mesh.shape["tp"]), ("z", "y", "c", "x"))
    placed = (
        P(FS, None),
        P(FS, "x"),
        P(FS, None),
        P(FS, "x"),
        P(FS, "x"),
        P(FS, "x"),
        P(FS, "x"),
        P(),
        P(),
        P(),
    )
    return jax.shard_map(
        local,
        mesh=split,
        in_specs=placed,
        out_specs=(P(FS, "x"),) * 5 + (P(),) * 4,
        check_vma=False,
    )
```

```python
import functools

import jax
import jax.numpy as jnp
from jax import lax
from jax.experimental import pallas as pl
from jax.experimental.pallas import tpu as pltpu
from jax.sharding import Mesh
from jax.sharding import PartitionSpec as P

D = 2048
W = 2048
R = 512
H = 16
FS = ("z", "y", "c")
PLANE = ("z", "y")
CHIPS = 64
CHUNK = 18
ROWS = CHIPS * CHUNK
SWAP = [(0, 1), (1, 0)]
BF = jnp.bfloat16
F32 = jnp.float32
VMEM = pl.BlockSpec(memory_space=pltpu.VMEM)


def call(body, outs, count, flops, moved, scratch=()):
    return pl.pallas_call(
        body,
        out_shape=outs,
        in_specs=[VMEM] * count,
        out_specs=jax.tree.map(lambda _: VMEM, outs),
        scratch_shapes=list(scratch),
        compiler_params=pltpu.CompilerParams(vmem_limit_bytes=12 << 20),
        cost_estimate=pl.CostEstimate(flops=flops, bytes_accessed=moved, transcendentals=0),
    )


def shape(dims, dtype):
    return jax.ShapeDtypeStruct(dims, dtype)


def decay_body(cot_ref, x_ref, out_ref, rows):
    part = jnp.dot(cot_ref[...], x_ref[...], preferred_element_type=F32)
    for b in range(D // 128):
        half, at = (b % 4) // 2, (b // 4) * 2 + b % 2
        rows[half, pl.ds(at, H, stride=8), :] = part[:, b * 128 : (b + 1) * 128]
    out_ref[...] = rows[...].astype(BF)


def project_body(x_ref, near_ref, far_ref, own_ref, out_ref, whole):
    core = lax.axis_index("c")
    whole[:, pl.ds(core, 1)] = near_ref[...].reshape(CHIPS, 1, 16, 128)
    whole[:, pl.ds(1 - core, 1)] = far_ref[...].reshape(CHIPS, 1, 16, 128)
    part = jnp.dot(
        x_ref[...], whole[...].reshape(D, 128), preferred_element_type=F32
    ).astype(BF)
    a = lax.broadcasted_iota(jnp.int32, (128, 128), 0)
    lane = lax.broadcasted_iota(jnp.int32, (128, 128), 1)
    half = jnp.where(a < 64, 1 - core, core)
    source = (a & 15) * 8 + half * 4 + ((a >> 4) & 3)
    order = jnp.where(lane == source, 1.0, 0.0).astype(BF)
    turned = lax.dot_general(
        order, part, (((1,), (1,)), ((), ())), preferred_element_type=F32
    ).astype(BF)
    out_ref[0:128, :] = turned
    out_ref[128:136, :] = jnp.zeros((8, 768), BF)
    out_ref[128:136, 0:128] = own_ref[0:8]
    out_ref[128:136, 128:256] = own_ref[8:16]


def gradient_body(half, p_ref, v_ref, dec_ref, out_ref, rows, dec):
    core = lax.axis_index("c")
    for q in range(4):
        part = jnp.dot(
            p_ref[q, half * 64 : half * 64 + 64, :], v_ref[...], preferred_element_type=F32
        )
        for i in range(4):
            for cb in range(4):
                rows[pl.ds(q * 16 * CHUNK + cb * 4 + i, 16, stride=CHUNK), :] = part[
                    i * 16 : i * 16 + 16, cb * 128 : cb * 128 + 128
                ]
    side = core if half == 1 else 1 - core
    dec[...] = dec_ref[side].astype(F32)
    for k in range(2):
        rows[pl.ds(16 + k, CHIPS, stride=CHUNK), :] = dec[pl.ds(k, CHIPS, stride=2), :]
    out_ref[...] = rows[...].astype(BF)


def copies_body(own_ref, out_ref):
    out_ref[...] = jnp.broadcast_to(own_ref[...][None], (CHIPS, 16, 128))


def pair_body(own_ref, peer_ref, out_ref):
    out_ref[...] = (own_ref[...].astype(F32) + peer_ref[...].astype(F32)).astype(BF)


def moment_body(got_ref, mean_ref, var_ref, out_ref, mean_out, var_out, mean_s, var_s, sums, new):
    for cb in range(4):
        lanes = slice(cb * 128, cb * 128 + 128)
        mean_s[cb * 4 : cb * 4 + 4, :] = mean_ref[:, lanes]
        var_s[cb * 4 : cb * 4 + 4, :] = var_ref[:, lanes]
    sums[...] = jnp.sum(got_ref[...].astype(F32).reshape(CHIPS // 4, 4 * CHUNK, 128), axis=0)
    total = (
        sums[0:CHUNK, :]
        + sums[CHUNK : 2 * CHUNK, :]
        + sums[2 * CHUNK : 3 * CHUNK, :]
        + sums[3 * CHUNK : 4 * CHUNK, :]
    )
    grad = total[0:16]
    mean_new = 0.9 * mean_s[...] + 0.1 * grad
    var_new = 0.95 * var_s[...] + 0.05 * grad * grad
    ratio = mean_new / (jnp.sqrt(var_new) + 1e-08)
    mean_s[...] = mean_new
    var_s[...] = var_new
    for cb in range(4):
        lanes = slice(cb * 128, cb * 128 + 128)
        mean_out[:, lanes] = mean_s[cb * 4 : cb * 4 + 4, :]
        var_out[:, lanes] = var_s[cb * 4 : cb * 4 + 4, :]
    for copy in range(8):
        new[copy * CHUNK : copy * CHUNK + 16, :] = ratio
        new[copy * CHUNK + 16 : copy * CHUNK + 18, :] = total[16:18]
    eight = new[...].astype(BF)
    for at in range(0, ROWS, 8 * CHUNK):
        out_ref[at : at + 8 * CHUNK, :] = eight


def spread_body(p_ref, out_ref):
    core = lax.axis_index("c")
    wide = 16 * CHUNK
    lane = lax.broadcasted_iota(jnp.int32, (128, wide), 0)
    k = lax.broadcasted_iota(jnp.int32, (128, wide), 1)
    chip = (k * 3641) >> 16
    row = k - chip * CHUNK
    mine = lax.broadcasted_iota(jnp.int32, (16, wide), 1)
    column = (mine - ((mine * 3641) >> 16) * CHUNK) >> 2
    for side in range(2):
        half = core if side == 0 else 1 - core
        hit = (lane == chip * 8 + half * 4 + (row & 3)) & (row < 16)
        pick = jnp.where(hit, 1.0, 0.0).astype(BF)
        for q in range(4):
            own = jnp.concatenate(
                [
                    p_ref[q, 128:136, 0:128].astype(F32),
                    p_ref[q, 128:136, 128:256].astype(F32),
                ]
            ).astype(BF)
            rows = jnp.dot(own, pick, preferred_element_type=F32)
            for cb in range(4):
                out_ref[side, q, cb * 16 : cb * 16 + 16, :] = jnp.where(
                    column == cb, rows, 0.0
                ).astype(BF)


def decay_update_body(
    near_ref,
    far_ref,
    weight_ref,
    mean_ref,
    var_ref,
    low_mean_ref,
    low_var_ref,
    new_out,
    copy_out,
    mean_out,
    var_out,
    low_mean_out,
    low_var_out,
    rows,
):
    low_mean_out[...] = low_mean_ref[...]
    low_var_out[...] = low_var_ref[...]
    core = lax.axis_index("c")
    rows[core] = near_ref[...].astype(F32)
    rows[1 - core] = far_ref[...].astype(F32)
    for b in range(D // 128):
        half, k = (b % 4) // 2, b % 2
        at = (b // 4) * CHUNK + 16 + k
        lanes = slice(b * 128, (b + 1) * 128)
        grad = rows[half, pl.ds(at, H, stride=4 * CHUNK), :]
        mean_new = 0.9 * mean_ref[:, lanes] + 0.1 * grad
        var_new = 0.95 * var_ref[:, lanes] + 0.05 * grad * grad
        new = weight_ref[:, lanes] - 0.5 * mean_new / (jnp.sqrt(var_new) + 1e-08)
        mean_out[:, lanes] = mean_new
        var_out[:, lanes] = var_new
        new_out[:, lanes] = new
        copy_out[:, lanes] = new.astype(BF)


def squares_body(near_ref, out_ref):
    near = near_ref[...].astype(F32).reshape(CHIPS // 4, 4 * CHUNK, 128)
    row = lax.broadcasted_iota(jnp.int32, (4 * CHUNK, 128), 0)
    row = row - ((row * 3641) >> 16) * CHUNK
    sums = jnp.where(row < 16, jnp.sum(near * near, axis=0), 0.0)
    sums = jnp.sum(sums, axis=0, keepdims=True)
    out_ref[...] = jnp.broadcast_to(sums[None], (8, 1, 128))


def product_body(rows_ref, near_ref, far_ref, out_ref):
    got = jnp.zeros((64, 128), F32)
    for q in range(4):
        part = slice(q * 16 * CHUNK, (q + 1) * 16 * CHUNK)
        got += jnp.dot(rows_ref[0, q], near_ref[part, :], preferred_element_type=F32)
        got += jnp.dot(rows_ref[1, q], far_ref[part, :], preferred_element_type=F32)
    for cb in range(4):
        out_ref[:, cb * 128 : cb * 128 + 128] = got[cb * 16 : cb * 16 + 16]


def step_body(squares_ref, delta_ref, weight_ref, step_out, new_out, copy_out):
    root_mean = jnp.sqrt(jnp.sum(squares_ref[...]) / (R * W) + 1e-06)
    step = -0.5 / root_mean * delta_ref[...]
    new = weight_ref[...] + step
    step_out[...] = step
    new_out[...] = new
    copy_out[...] = new.astype(BF)


def local(
    inputs,
    values_cot,
    decay_cot,
    factor,
    value_weight,
    lowrank_mean,
    lowrank_var,
    decay_weight,
    decay_mean,
    decay_var,
):
    chunk = shape((ROWS, 128), BF)

    def across(rows):
        tiles = rows.reshape(CHIPS, CHUNK // 2, 2, 128)
        return lax.all_to_all(tiles, PLANE, 0, 0, tiled=True).reshape(ROWS, 128)

    copies = call(copies_body, shape((CHIPS, 16, 128), BF), 1, 0, 1 << 18)(factor)
    near = lax.all_to_all(copies, PLANE, 0, 0, tiled=True)
    decay_rows = call(
        decay_body,
        shape((2, CHIPS * 2, 128), BF),
        2,
        2 * 768 * D * H,
        4 << 20,
        [pltpu.VMEM((2, CHIPS * 2, 128), F32)],
    )(decay_cot.T, inputs)
    near, decay_rows = lax.optimization_barrier((near, decay_rows))
    far = lax.ppermute(near, "c", SWAP)
    quarter = call(
        project_body,
        shape((136, 768), BF),
        4,
        2 * 768 * D * 128,
        4 << 20,
        [pltpu.VMEM((CHIPS, 2, 16, 128), BF)],
    )(inputs, near, far, factor)
    projected = lax.all_gather(quarter, "x")

    def gradient(half):
        return call(
            functools.partial(gradient_body, half),
            chunk,
            3,
            2 * 768 * 256 * 512,
            2 << 20,
            [pltpu.VMEM((ROWS, 128), F32), pltpu.VMEM((CHIPS * 2, 128), F32)],
        )(projected, values_cot, decay_rows)

    theirs = gradient(0)
    peer = lax.ppermute(theirs, "c", SWAP)
    paired = call(pair_body, chunk, 2, 400000, 1 << 20)(gradient(1), peer)
    arrived = across(paired)
    rows = call(spread_body, shape((2, 4, 64, 16 * CHUNK), BF), 1, 8 * 2 * 16 * 128 * 256, 1 << 20)(
        projected
    )
    ratio, mean_new, var_new = call(
        moment_body,
        (chunk, pltpu.VMEM((4, 512), F32), pltpu.VMEM((4, 512), F32)),
        3,
        400000,
        1 << 20,
        [
            pltpu.VMEM((16, 128), F32),
            pltpu.VMEM((16, 128), F32),
            pltpu.VMEM((4 * CHUNK, 128), F32),
            pltpu.VMEM((8 * CHUNK, 128), F32),
        ],
    )(arrived, lowrank_mean, lowrank_var)
    near = across(ratio)
    far = lax.ppermute(near, "c", SWAP)
    state = shape((H, D), F32)
    low = shape((4, 512), F32)
    (decay_new, decay_copy, decay_mean_new, decay_var_new, mean_new, var_new) = call(
        decay_update_body,
        (state, shape((H, D), BF), state, state, low, low),
        7,
        400000,
        1 << 20,
        [pltpu.VMEM((2, ROWS, 128), F32)],
    )(near, far, decay_weight.T, decay_mean.T, decay_var.T, mean_new, var_new)
    squares = call(squares_body, shape((8, 1, 128), F32), 1, 400000, 1 << 20)(near)
    squares = lax.all_to_all(squares, ("c", "x"), 0, 0, tiled=True)
    delta = call(
        product_body, shape((16, 512), F32), 3, 2 * 64 * 2048 * 128, 1 << 20
    )(rows, near, far)
    block = shape((16, 512), F32)
    value_step, value_new, value_copy = call(
        step_body, (block, block, shape((16, 512), BF)), 3, 40000, 100000
    )(squares, delta, value_weight)
    return (
        value_step,
        value_new,
        value_copy,
        mean_new,
        var_new,
        decay_new.T,
        decay_copy.T,
        decay_mean_new.T,
        decay_var_new.T,
    )


def solution(mesh):
    split = Mesh(mesh.devices.reshape(8, 8, 2, mesh.shape["tp"]), ("z", "y", "c", "x"))
    placed = (
        P(FS, None),
        P(FS, "x"),
        P(FS, None),
        P(FS, "x"),
        P(FS, "x"),
        P(FS, "x"),
        P(FS, "x"),
        P(),
        P(),
        P(),
    )
    return jax.shard_map(
        local,
        mesh=split,
        in_specs=placed,
        out_specs=(P(FS, "x"),) * 5 + (P(),) * 4,
        check_vma=False,
    )
```
